32 devices in a mesh: ep: 8 (over z, x), tp: 4 (over y, core).
Axes of the slice: x: 2, y: 2, z: 4, core: 2. Of those that a mesh axis runs over, the one named last changes fastest.
Arguments:
- tokens: bfloat16 [4096, 4096], P('ep', 'tp'), may hold values from -60 to 60
- routes: int32 [4096, 4], P('ep'), may hold values from 0 to 31, all different within a row; in each aligned block of 512 rows (0 to 511, 512 to 1023, ...) at most 128 rows name the same one
- route_weights: float32 [4096, 4], P('ep'), may hold values from 0.1 to 1
- pre_gain: float32 [4096], P('tp'), may hold values from 0.1 to 1.9
- expert_gate: bfloat16 [32, 4096, 512], P('ep', 'tp'), may hold values from -0.09375 to 0.09375
- expert_up: bfloat16 [32, 4096, 512], P('ep', 'tp'), may hold values from -0.09375 to 0.09375
- expert_down: bfloat16 [32, 512, 4096], P('ep', None, 'tp'), may hold values from -1 to 1
- shared_gate: bfloat16 [4096, 512], P('tp'), may hold values from -0.09375 to 0.09375
- shared_up: bfloat16 [4096, 512], P('tp'), may hold values from -0.09375 to 0.09375
- shared_down: bfloat16 [512, 4096], P(None, 'tp'), may hold values from -1 to 1
- post_gain: float32 [4096], P('tp'), may hold values from 0.1 to 1.9
Outputs:
- layer_out: bfloat16 [4096, 4096], P('ep', 'tp')
The draws below stay inside these ranges and needn't reach their ends.
Inputs may be any that keep to these rules, and one draw needn't show every extreme that they name: `routes`: each row names 4 different experts. Within each aligned block of 512 rows (the tokens of one index of ep) no expert is named more than 128 times, a bound that some block reaches.
All inputs are finite; a program needn't handle non-finite values.
Results may differ from the reference program's by a relative error of at most 0.022.
Values may be sent and summed in bfloat16 or wider, within the bound.
A program may use at most 128 MiB of HBM per device.

```python
import math
import jax
import jax.numpy as jnp
import numpy as np
from jax import lax

D = 4096
FF = 512
FS = 512
TOPK = 4
TOK_EP = 512
EXPERTS = 32
TOKENS = 4096
CAP = 128
N_EP = 8
N_TP = 4


def draw_tokens(key, part):
    key_base, key_rows, key_cols = jax.random.split(key, 3)
    ramp = 3.0 ** (jnp.arange(D, dtype=jnp.float32) / D)
    columns = ramp * jax.random.uniform(key_cols, (D,), jnp.float32, 0.5, 2.0)
    scales = jnp.exp(jax.random.uniform(key_rows, (TOKENS, 1), jnp.float32, -1.0, 1.0))
    base = jnp.clip(jax.random.normal(key_base, (TOKENS, D), jnp.float32), -6.0, 6.0)
    return jnp.clip(base * scales * columns, -60.0, 60.0).astype(jnp.bfloat16)


def ramped_weight(key, shape, fan_in):
    key_base, key_cols = jax.random.split(key)
    ramp = 3.0 ** (jnp.arange(D, dtype=jnp.float32) / D)
    columns = ramp * jax.random.uniform(key_cols, (D,), jnp.float32, 0.5, 2.0) / 2.0
    base = jnp.clip(jax.random.normal(key_base, shape, jnp.float32), -6.0, 6.0) * fan_in ** (-0.5)
    return jnp.clip(base * columns, -1.0, 1.0).astype(jnp.bfloat16)


def draw_expert_down(key, part):
    return ramped_weight(key, (EXPERTS, FF, D), FF)


def draw_shared_down(key, part):
    return ramped_weight(key, (FS, D), FS)


def steps_of(rng, dims, cuts, low, top_value):
    def one(position, shards_of):
        steps = jax.random.uniform(jax.random.fold_in(jax.random.fold_in(rng, 6), position), (shards_of,), jnp.float32, low / len(cuts), top_value / len(cuts))
        return jnp.repeat(jnp.exp(steps), dims[position] // shards_of).reshape((-1,) + (1,) * (len(dims) - position - 1))

    factor_of = one(*cuts[0])
    for cut in cuts[1:]:
        factor_of = factor_of * one(*cut)
    return factor_of


def routed_block(rng, own, number, rows, number_of, top, limit, slope):
    ranking = jax.random.permutation(rng, number_of)
    heavy_load, usual = shares(number_of, rows * top, limit, slope, True), shares(number_of, rows * top, limit, slope, False)
    places = jnp.arange(number_of)

    def named(sizes, offset_by):
        used = int((sizes > 0).sum())
        fixed = max(1, used // 4)
        moved = fixed + (places - fixed + offset_by * (used - fixed)) % max(1, number_of - fixed)
        return jnp.zeros((number_of,), jnp.int32).at[ranking[jnp.where(places < fixed, places, moved)]].set(jnp.asarray(sizes, jnp.int32))

    sizes = jnp.where(number % 4 == 0, named(heavy_load, number // 4), named(usual, number - number // 4 - 1))
    mixed = jax.random.permutation(jax.random.fold_in(own, 3), number_of)
    source_of, sink = mixed[0:number_of // 2 * 2:2], mixed[1:number_of // 2 * 2:2]
    slack = jnp.minimum(sizes[source_of] - 1, limit - sizes[sink]) // 2
    slack = jnp.where((source_of == ranking[0]) | (sink == ranking[0]) | (sizes[sink] == 0), 0, jnp.maximum(slack, 0))
    moved = jax.random.randint(jax.random.fold_in(own, 4), (number_of // 2,), 0, 1 << 20) % (slack + 1)
    sizes = sizes.at[source_of].add(-moved).at[sink].add(moved)
    labels = jnp.searchsorted(jnp.cumsum(sizes), jnp.arange(rows * top), side="right").astype(jnp.int32)
    table = labels.reshape(top, rows).T
    table = table[jax.random.permutation(jax.random.fold_in(own, 1), rows)]
    offset_by = jax.random.randint(jax.random.fold_in(own, 2), (rows, 1), 0, top)
    return jnp.take_along_axis(table, (jnp.arange(top)[None, :] + offset_by) % top, axis=1)


def shares(count, total, reach, lean, full):
    portions = [(1 << 20) // math.isqrt(grade ** lean) + 1 for grade in range(1, count + 1)]
    largest = reach if full else min(reach, max(-(-total // count), total * portions[0] // sum(portions)))
    least = 1 if total - largest >= count - 1 else 0
    counts, surplus = [largest] + [least] * (count - 1), total - largest - least * (count - 1)
    while surplus > 0:
        candidates = [i for i in range(1, count) if counts[i] < largest] or [i for i in range(1, count) if counts[i] < reach]
        mass, budget = sum([portions[i] for i in candidates]), surplus
        for i in candidates:
            extra = min(reach - counts[i], max(1, budget * portions[i] // mass), surplus)
            counts[i] = counts[i] + extra
            surplus = surplus - extra
    return np.array(counts)


def centred(rng, shape, width, reach, cuts=(), kind=jnp.bfloat16):
    gain = steps_of(rng, shape, cuts, -0.22, 0.18) if cuts else 1.0
    drawn = jax.random.normal(rng, shape, jnp.float32) * width * gain
    return jnp.minimum(jnp.maximum(drawn, -reach), reach).astype(kind)


def setup_inputs(seed: int = 0) -> dict:
    streams_of = jax.random.split(jax.random.key(seed), 12)
    tokens = draw_tokens(jax.random.fold_in(streams_of[11], 71), 0)
    routes_keys = jax.random.split(jax.random.fold_in(streams_of[1], 1), TOKENS // TOK_EP)
    routes_turns = jax.random.permutation(jax.random.fold_in(streams_of[1], 3), TOKENS // TOK_EP)
    routes = jax.vmap(lambda own, number: routed_block(jax.random.fold_in(streams_of[1], 2), own, number, TOK_EP, EXPERTS, TOPK, CAP, 2))(routes_keys, routes_turns).reshape((TOKENS, TOPK))
    route_weights = jnp.clip(jnp.exp(math.log(1.0) - 2.3025851 * jax.random.uniform(streams_of[2], (TOKENS, TOPK), jnp.float32) ** steps_of(streams_of[2], (TOKENS, TOPK), ((0, 8),), -0.2, 0.2)), 0.1, 1.0)
    pre_gain = jnp.clip(1.0 + 0.18 * jax.random.normal(streams_of[3], (D,), jnp.float32), 0.1, 1.9)
    expert_gate = centred(streams_of[4], (EXPERTS, D, FF), D ** -0.5, 0.09375, ((0, 8), (1, 4)))
    expert_up = centred(streams_of[5], (EXPERTS, D, FF), D ** -0.5, 0.09375, ((0, 8), (1, 4)))
    expert_down = draw_expert_down(jax.random.fold_in(streams_of[11], 71), 0)
    shared_gate = centred(streams_of[7], (D, FS), D ** -0.5, 0.09375, ((0, 4),))
    shared_up = centred(streams_of[8], (D, FS), D ** -0.5, 0.09375, ((0, 4),))
    shared_down = draw_shared_down(jax.random.fold_in(streams_of[11], 71), 0)
    post_gain = jnp.clip(1.0 + 0.18 * jax.random.normal(streams_of[10], (D,), jnp.float32), 0.1, 1.9)
    return {"tokens": tokens, "routes": routes, "route_weights": route_weights, "pre_gain": pre_gain, "expert_gate": expert_gate, "expert_up": expert_up, "expert_down": expert_down, "shared_gate": shared_gate, "shared_up": shared_up, "shared_down": shared_down, "post_gain": post_gain}


epsilon = 1e-06

def inverse_norm(values):
    return lax.rsqrt(lax.optimization_barrier(jnp.mean(values * values, axis=1)) + epsilon)

def blocked_product(inputs, weight):
    row_count = inputs.shape[0]
    out_width = weight.shape[1]
    pieces = inputs.reshape(row_count, N_TP, D // N_TP).astype(jnp.float32)
    blocks = weight.reshape(N_TP, D // N_TP, out_width).astype(jnp.float32)
    partial_value = jnp.einsum('rnd,ndf->nrf', pieces, blocks)
    rounded = lax.optimization_barrier(partial_value.astype(jnp.bfloat16))
    return lax.optimization_barrier(jnp.sum(rounded.astype(jnp.float32), axis=0))

def reference(tokens, routes, route_weights, pre_gain, expert_gate, expert_up, expert_down, shared_gate, shared_up, shared_down, post_gain):
    inputs = tokens.astype(jnp.float32)
    normed = (inputs * inverse_norm(inputs)[:, None] * pre_gain.astype(jnp.float32)).astype(jnp.bfloat16)
    per_block = TOK_EP * TOPK
    flat_ids = routes.reshape(N_EP, per_block).astype(jnp.int32)
    one_hot = (flat_ids[:, :, None] == jnp.arange(EXPERTS, dtype=jnp.int32)[None, None, :]).astype(jnp.int32)
    slots = lax.optimization_barrier(jnp.sum(jnp.cumsum(one_hot, axis=1) * one_hot, axis=2)) - 1
    sources = jnp.arange(N_EP, dtype=jnp.int32)[:, None]
    positions = (sources * CAP + slots).reshape(-1).astype(jnp.int32)
    token_index = (sources * TOK_EP + jnp.arange(per_block, dtype=jnp.int32)[None, :] // TOPK).reshape(-1).astype(jnp.int32)
    expert_index = flat_ids.reshape(-1)
    token_table = jnp.full((EXPERTS, N_EP * CAP), TOKENS, jnp.int32).at[expert_index, positions].set(token_index)
    weight_table = jnp.zeros((EXPERTS, N_EP * CAP), jnp.float32).at[expert_index, positions].set(route_weights.reshape(-1).astype(jnp.float32))

    def expert_step(totals, stacked):
        table_rows, table_weights, gate_weight, up_weight, down_weight = stacked
        arrived = jnp.take(normed, table_rows, axis=0, mode='fill', fill_value=0)
        gate_pre = blocked_product(arrived, gate_weight)
        up_pre = blocked_product(arrived, up_weight)
        hidden = (jax.nn.silu(gate_pre) * up_pre).astype(jnp.bfloat16)
        expert_out = jnp.dot(hidden, down_weight, preferred_element_type=jnp.float32).astype(jnp.bfloat16)
        totals = totals.at[table_rows].add(table_weights[:, None] * expert_out.astype(jnp.float32), mode='drop')
        return (totals, None)
    routed, _ = lax.scan(expert_step, jnp.zeros((TOKENS, D), jnp.float32), (token_table, weight_table, expert_gate, expert_up, expert_down))
    shared_gate_pre = blocked_product(normed, shared_gate)
    shared_up_pre = blocked_product(normed, shared_up)
    shared_hidden = (jax.nn.silu(shared_gate_pre) * shared_up_pre).astype(jnp.bfloat16)
    shared_out = jnp.dot(shared_hidden, shared_down, preferred_element_type=jnp.float32).astype(jnp.bfloat16)
    mixture = routed + shared_out.astype(jnp.float32)
    return (mixture * inverse_norm(mixture)[:, None] * post_gain.astype(jnp.float32)).astype(jnp.bfloat16)
```

```python
import jax
import jax.numpy as jnp
from jax import lax
from jax.experimental import pallas as pl
from jax.experimental.pallas import tpu as pltpu
from jax.sharding import PartitionSpec as P


epsilon = 1e-06
SLOT, WEIGHT, INVERSE = 0, 1, 2


def ring_of(groups, width):
    if width < 2 or groups % width or groups // width < 2:
        return list(range(groups))
    depth = groups // width
    cycle = []
    for x in range(width):
        column = range(1, depth) if x % 2 == 0 else range(depth - 1, 0, -1)
        cycle += [z * width + x for z in column]
    return cycle + [x for x in range(width - 1, -1, -1)]


def bit_reversed(count):
    order = [0]
    step = count // 2
    while step >= 1:
        order = order + [p + step for p in order]
        step //= 2
    return order


def one_hot(meta_ref, capacity):
    slot = meta_ref[0, 0, SLOT : SLOT + 1, :]
    rows = lax.broadcasted_iota(jnp.int32, (capacity, slot.shape[1]), 0).astype(jnp.float32)
    return rows == slot


def row_value(hit, meta_ref, which):
    values = meta_ref[0, 0, which : which + 1, :]
    return jnp.sum(jnp.where(hit, values, 0.0), axis=1, keepdims=True)


def dispatch_kernel(blocks, capacity, *refs):
    metas, inputs = refs[:blocks], refs[blocks : 2 * blocks]
    gain_ref, send_weight, keep_weight, send_ref, keep_ref = refs[2 * blocks :]
    parts = []
    for meta_ref, x_ref in zip(metas, inputs):
        hit = one_hot(meta_ref, capacity)
        picked = jnp.dot(
            jnp.where(hit, 1.0, 0.0).astype(jnp.bfloat16),
            x_ref[...],
            preferred_element_type=jnp.float32,
        )
        scaled = picked * row_value(hit, meta_ref, INVERSE) * gain_ref[...]
        parts.append(scaled.astype(jnp.bfloat16))
    rows = parts[0] if blocks == 1 else jnp.concatenate(parts, axis=0)
    send_ref[0] = jnp.dot(rows, send_weight[0], preferred_element_type=jnp.float32).astype(
        jnp.bfloat16
    )
    keep_ref[0] = jnp.dot(rows, keep_weight[0], preferred_element_type=jnp.float32).astype(
        jnp.bfloat16
    )


def combine_kernel(blocks, capacity, *refs):
    metas = refs[:blocks]
    hidden_ref, down_ref = refs[blocks : blocks + 2]
    outs = refs[blocks + 2 : 2 * blocks + 2]
    totals = refs[2 * blocks + 2]
    expert = pl.program_id(0)
    produced = jnp.dot(hidden_ref[0], down_ref[0], preferred_element_type=jnp.float32)
    for b in range(blocks):
        hit = one_hot(metas[b], capacity)
        rows = produced[b * capacity : (b + 1) * capacity] * row_value(hit, metas[b], WEIGHT)
        added = lax.dot_general(
            jnp.where(hit, 1.0, 0.0).astype(jnp.bfloat16),
            rows.astype(jnp.bfloat16),
            (((0,), (0,)), ((), ())),
            preferred_element_type=jnp.float32,
        )

        @pl.when(expert == 0)
        def _():
            totals[b] = added

        @pl.when(expert > 0)
        def _():
            totals[b] += added

        @pl.when(expert == pl.num_programs(0) - 1)
        def _():
            outs[b][...] = totals[b].astype(jnp.bfloat16)


def meta_specs(first, blocks, meta):
    shape = (1, 1) + meta.shape[2:]
    return [
        pl.BlockSpec(shape, lambda e, at=first + b: (at, e, 0, 0)) for b in range(blocks)
    ]


def dispatch(first, inputs, meta, capacity, gain, send_weight, keep_weight):
    blocks = len(inputs)
    experts, depth, width = send_weight.shape
    rows = blocks * capacity
    whole = lambda e: (0, 0)
    own = lambda e: (e, 0, 0)
    out = jax.ShapeDtypeStruct((experts, rows, width), jnp.bfloat16)
    flops = 2 * experts * (rows * depth * width * 2 + rows * inputs[0].shape[0] * depth)
    return pl.pallas_call(
        lambda *refs: dispatch_kernel(blocks, capacity, *refs),
        grid=(experts,),
        in_specs=meta_specs(first, blocks, meta)
        + [pl.BlockSpec(x.shape, whole) for x in inputs]
        + [pl.BlockSpec(gain.shape, whole)]
        + [pl.BlockSpec((1, depth, width), own)] * 2,
        out_specs=[pl.BlockSpec((1, rows, width), own)] * 2,
        out_shape=[out, out],
        cost_estimate=pl.CostEstimate(
            flops=flops, bytes_accessed=4 * send_weight.size + 4 * rows * depth, transcendentals=0
        ),
        name="dispatch",
    )(*([meta] * blocks), *inputs, gain, send_weight, keep_weight)


def combine(first, blocks, hidden, meta, capacity, down):
    experts, rows, units = hidden.shape
    width = down.shape[2]
    tokens = meta.shape[3]
    own = lambda e: (e, 0, 0)
    out = jax.ShapeDtypeStruct((tokens, width), jnp.bfloat16)
    flops = 2 * experts * (rows * units * width + rows * tokens * width)
    return pl.pallas_call(
        lambda *refs: combine_kernel(blocks, capacity, *refs),
        grid=(experts,),
        in_specs=meta_specs(first, blocks, meta)
        + [pl.BlockSpec((1, rows, units), own), pl.BlockSpec((1, units, width), own)],
        out_specs=[pl.BlockSpec((tokens, width), lambda e: (0, 0))] * blocks,
        out_shape=[out] * blocks,
        scratch_shapes=[pltpu.VMEM((blocks, tokens, width), jnp.float32)],
        cost_estimate=pl.CostEstimate(
            flops=flops, bytes_accessed=2 * down.size + 8 * tokens * width, transcendentals=0
        ),
        name="combine",
    )(*([meta] * blocks), hidden, down)


def flipped(value, bit, members):
    return lax.ppermute(value, "tp", [(j, j ^ bit) for j in range(members)])


def exchange(send, keep, members):
    bit = 1
    total = keep.astype(jnp.float32)
    while bit < members:
        total = total + flipped(send, bit, members).astype(jnp.float32)
        bit *= 2
        if bit < members:
            half = total.shape[1] // 2
            total, send = total[:, :half], total[:, half:].astype(jnp.bfloat16)
    share = total.shape[1] // 2
    hidden = (jax.nn.silu(total[:, :share]) * total[:, share:]).astype(jnp.bfloat16)
    while bit > 1:
        bit //= 2
        hidden = jnp.concatenate([hidden, flipped(hidden, bit, members)], axis=1)
    return hidden


def sum_squares(values):
    return lax.psum(jnp.sum(values * values, axis=1), "tp")


def per_device(
    tokens,
    routes,
    route_weights,
    pre_gain,
    expert_gate,
    expert_up,
    expert_down,
    shared_gate,
    shared_up,
    shared_down,
    post_gain,
):
    members, groups = lax.axis_size("tp"), lax.axis_size("ep")
    me, group = lax.axis_index("tp"), lax.axis_index("ep")
    count, width = tokens.shape
    fanout = routes.shape[1]
    features = width * members
    experts = expert_gate.shape[0]
    capacity = 2 * count * fanout // (experts * groups)

    ring = ring_of(groups, members // 2)
    ahead = [(ring[i], ring[(i + 1) % groups]) for i in range(groups)]
    behind = [(b, a) for a, b in ahead]
    reach = groups // 2
    half = width // 2

    before, after = [tokens], [tokens]
    for step in range(1, reach):
        before.append(lax.ppermute(before[-1], "ep", ahead))
        after.append(lax.ppermute(after[-1], "ep", behind))
    far = jnp.concatenate(
        [
            lax.ppermute(before[-1][:, :half], "ep", ahead),
            lax.ppermute(after[-1][:, half:], "ep", behind),
        ],
        axis=1,
    )

    inputs = tokens.astype(jnp.float32)
    inverse = lax.rsqrt(sum_squares(inputs) / features + epsilon)
    packed = jnp.concatenate(
        [routes.astype(jnp.float32), route_weights, inverse[:, None]], axis=1
    ).T
    gathered = lax.all_gather(packed, "ep", axis=0)
    relative = []
    for place in range(groups):
        offsets = [0]
        for step in range(1, reach):
            offsets += [-step, step]
        offsets.append(reach)
        relative.append([ring[(place + o) % groups] for o in offsets])
    table = [None] * groups
    for place in range(groups):
        table[ring[place]] = relative[place]
    gathered = gathered[jnp.array(table, jnp.int32)[group]]
    named = gathered[:, :fanout]
    mine = (group * experts + jnp.arange(experts, dtype=jnp.int32)).astype(jnp.float32)
    same = named[:, None] == mine[None, :, None, None]
    present = jnp.any(same, axis=2)
    weight = jnp.sum(jnp.where(same, gathered[:, None, fanout : 2 * fanout], 0.0), axis=2)
    positions = jnp.arange(count, dtype=jnp.int32)
    earlier = (positions[:, None] < positions[None, :]).astype(jnp.bfloat16)
    slots = jnp.dot(
        present.astype(jnp.bfloat16).reshape(groups * experts, count),
        earlier,
        preferred_element_type=jnp.float32,
    ).reshape(present.shape)
    meta = jnp.stack(
        [
            jnp.where(present, slots, -1.0),
            weight,
            jnp.broadcast_to(gathered[:, None, 2 * fanout], present.shape),
        ],
        axis=2,
    )

    order = bit_reversed(members)

    def pieces(array, axis, positions):
        size = array.shape[axis] // members
        return [
            lax.dynamic_slice_in_dim(array, (me ^ p) * size, size, axis) for p in positions
        ]

    def interleaved(gate, up, positions):
        axis = gate.ndim - 1
        pairs = zip(pieces(gate, axis, positions), pieces(up, axis, positions))
        return jnp.concatenate([x for pair in pairs for x in pair], axis=axis)

    kept, sent = order[: members // 2], order[members // 2 :]
    send_weight = interleaved(expert_gate, expert_up, sent)
    keep_weight = interleaved(expert_gate, expert_up, kept)
    down = jnp.concatenate(pieces(expert_down, 1, order), axis=1)
    shared_send = interleaved(shared_gate, shared_up, sent)
    shared_keep = interleaved(shared_gate, shared_up, kept)
    shared_last = jnp.concatenate(pieces(shared_down, 0, order), axis=0)
    gain = pre_gain[None, :]

    normed = (inputs * inverse[:, None] * pre_gain).astype(jnp.bfloat16)
    send, keep = dispatch(0, [tokens], meta, capacity, gain, send_weight, keep_weight)
    own_rows = experts * capacity
    send = jnp.concatenate(
        [
            send.reshape(own_rows, -1),
            jnp.dot(normed, shared_send, preferred_element_type=jnp.float32).astype(jnp.bfloat16),
        ],
        axis=0,
    )
    keep = jnp.concatenate(
        [
            keep.reshape(own_rows, -1),
            jnp.dot(normed, shared_keep, preferred_element_type=jnp.float32).astype(jnp.bfloat16),
        ],
        axis=0,
    )
    hidden = exchange(send, keep, members)
    (own,) = combine(
        0, 1, hidden[:own_rows].reshape(experts, capacity, -1), meta, capacity, down
    )
    shared_out = jnp.dot(hidden[own_rows:], shared_last, preferred_element_type=jnp.float32)

    def stage(first, blocks):
        send, keep = dispatch(first, blocks, meta, capacity, gain, send_weight, keep_weight)
        rows = experts * len(blocks) * capacity
        hidden = exchange(send.reshape(rows, -1), keep.reshape(rows, -1), members)
        return combine(
            first,
            len(blocks),
            hidden.reshape(experts, len(blocks) * capacity, -1),
            meta,
            capacity,
            down,
        )

    back, forth = [None], [None]
    for step in range(1, reach):
        from_before, from_after = stage(2 * step - 1, [before[step], after[step]])
        back.append(from_before)
        forth.append(from_after)
    (far_out,) = stage(2 * reach - 1, [far])

    def added(a, b):
        return (a.astype(jnp.float32) + b.astype(jnp.float32)).astype(jnp.bfloat16)

    up_half = lax.ppermute(far_out[:, :half], "ep", ahead)
    down_half = lax.ppermute(far_out[:, half:], "ep", behind)
    for step in range(reach - 1, 0, -1):
        if step == reach - 1:
            zero = jnp.zeros_like(up_half)
            ups = added(forth[step], jnp.concatenate([up_half, zero], axis=1))
            downs = added(back[step], jnp.concatenate([zero, down_half], axis=1))
        else:
            ups = added(forth[step], ups)
            downs = added(back[step], downs)
        ups = lax.ppermute(ups, "ep", ahead)
        downs = lax.ppermute(downs, "ep", behind)
    mixture = (
        own.astype(jnp.float32)
        + shared_out
        + ups.astype(jnp.float32)
        + downs.astype(jnp.float32)
    )
    scale = lax.rsqrt(sum_squares(mixture) / features + epsilon)
    return (mixture * scale[:, None] * post_gain).astype(jnp.bfloat16)


def solution(mesh):
    in_specs = (
        P("ep", "tp"),
        P("ep", None),
        P("ep", None),
        P("tp"),
        P("ep", "tp", None),
        P("ep", "tp", None),
        P("ep", None, "tp"),
        P("tp", None),
        P("tp", None),
        P(None, "tp"),
        P("tp"),
    )
    out_specs = P("ep", "tp")
    return jax.shard_map(
        per_device, mesh=mesh, in_specs=in_specs, out_specs=out_specs, check_vma=False
    )
```
